32 devices in a mesh: sp: 4 (over z), tp: 4 (over y, x), dp: 2 (over core).
Axes of the slice: x: 2, y: 2, z: 4, core: 2. Of those that a mesh axis runs over, the one named last changes fastest.
Arguments:
- latent_tokens: bfloat16 [4096, 2048], P(('dp', 'sp', 'tp')), parts along dimension 0, may hold values from -6 to 6
- condition: bfloat16 [4096], P(('dp', 'sp')), parts along dimension 0, may hold values from -6 to 6
- shift_weight: bfloat16 [2048, 2048], P('sp', 'tp'), may hold values from -0.125 to 0.125
- scale_weight: bfloat16 [2048, 2048], P('sp', 'tp'), may hold values from -0.125 to 0.125
- gate_weight: bfloat16 [2048, 2048], P('sp', 'tp'), may hold values from -0.125 to 0.125
- norm_gain: float32 [2048], replicated, may hold values from 0.1 to 1.9
- query_down: bfloat16 [2048, 512], replicated, may hold values from -0.125 to 0.125
- query_gain: float32 [512], replicated, may hold values from 0.1 to 1.9
- kv_down: bfloat16 [2048, 256], replicated, may hold values from -0.125 to 0.125
- kv_gain: float32 [256], replicated, may hold values from 0.1 to 1.9
- rope_down: bfloat16 [2048, 32], replicated, may hold values from -0.125 to 0.125
- query_up: bfloat16 [512, 1536], P(None, 'tp'), may hold values from -0.25 to 0.25
- key_up: bfloat16 [256, 1024], P(None, 'tp'), may hold values from -0.375 to 0.375
- value_up: bfloat16 [256, 1024], P(None, 'tp'), may hold values from -0.375 to 0.375
- query_norm_gain: float32 [96], replicated, may hold values from 0.47 to 16
- key_norm_gain: float32 [96], replicated, may hold values from 0.47 to 16
- out_weight: bfloat16 [1024, 2048], P('tp'), may hold values from -0.1875 to 0.1875
- context_latent: bfloat16 [2048, 256], P(('dp', 'sp')), parts along dimension 0, may hold values from -6 to 6
- context_rope: bfloat16 [2048, 32], P(('dp', 'sp')), parts along dimension 0, may hold values from -6 to 6
- context_lift: float32 [16], P('tp'), may hold values from 0 to 2
Outputs:
- output: bfloat16 [4096, 2048], P(('dp', 'sp', 'tp')), parts along dimension 0
The draws below stay inside these ranges and needn't reach their ends.
There are 2 independent parts, one for each index of `dp`. The reference program is written for one: setup_inputs(seed, part) draws one part's arguments, and reference() takes and returns one part's arrays. A program takes and returns all parts, laid end to end along the dimension named above; an argument that names none is the same for every part. Nothing has to cross between parts.
All inputs are finite; a program needn't handle non-finite values.
Results may differ from the reference program's by a relative error of at most 0.015.
The reference program's roundings to bfloat16 on the way count: a program that leaves them out, or rounds other values in their place, can miss the bound.
Values may be sent and summed in bfloat16 or wider, within the bound.
A program may use at most 128 MiB of HBM per device.

```python
import jax
import jax.numpy as jnp
from jax import lax

D_MODEL = 2048
HEADS = 16
NOPE_DIM = 64
ROPE_DIM = 32
VALUE_DIM = 64
QK_DIM = 96
Q_RANK = 512
KV_RANK = 256
GRID_W = 64
CONTEXT = 1024
TOKENS = 2048
N_TP = 4


def gain_draw(key, salt):
    own_key = jax.random.fold_in(key, salt)
    normal_values = jax.random.normal(own_key, (QK_DIM,), jnp.float32)
    return 1.7 * (1.0 + 0.18 * jnp.clip(normal_values, -4.0, 4.0))


def draw_query_norm_gain(key, part):
    return gain_draw(key, 31)


def draw_key_norm_gain(key, part):
    return gain_draw(key, 57)


def block_scale(rng, dims, cuts, least, top_value):
    loudness = 1.0
    for dim, shards_of in cuts:
        heights = jax.random.uniform(jax.random.fold_in(jax.random.fold_in(rng, 6), dim), (shards_of,), jnp.float32, least / len(cuts), top_value / len(cuts))
        loudness = loudness * jnp.repeat(jnp.exp(heights), dims[dim] // shards_of).reshape((-1,) + (1,) * (len(dims) - 1 - dim))
    return loudness


def bell_draw(key, shape, spread, bound, shards=(), kind=jnp.bfloat16):
    drawn = spread * jax.random.normal(key, shape, jnp.float32)
    if shards:
        drawn = drawn * block_scale(key, shape, shards, -0.22, 0.18)
    return jnp.clip(drawn, -bound, bound).astype(kind)


def setup_inputs(seed: int = 0, part: int = 0) -> dict:
    key_of = jax.random.split(jax.random.key(seed), 21)
    part_keys = jax.random.split(jax.random.fold_in(key_of[20], part), 21)
    latent_tokens = bell_draw(part_keys[0], (TOKENS, D_MODEL), 1.0, 6.0, ((0, 16),))
    condition = bell_draw(part_keys[1], (D_MODEL,), 1.0, 6.0, ((0, 4),))
    shift_weight = bell_draw(key_of[2], (D_MODEL, D_MODEL), D_MODEL ** -0.5, 0.125, ((0, 4), (1, 4)))
    scale_weight = bell_draw(key_of[3], (D_MODEL, D_MODEL), D_MODEL ** -0.5, 0.125, ((0, 4), (1, 4)))
    gate_weight = bell_draw(key_of[4], (D_MODEL, D_MODEL), D_MODEL ** -0.5, 0.125, ((0, 4), (1, 4)))
    norm_gain = jnp.clip(1.0 + 0.18 * jax.random.normal(key_of[5], (D_MODEL,), jnp.float32), 0.1, 1.9)
    query_down = bell_draw(key_of[6], (D_MODEL, Q_RANK), D_MODEL ** -0.5, 0.125)
    query_gain = jnp.clip(1.0 + 0.18 * jax.random.normal(key_of[7], (Q_RANK,), jnp.float32), 0.1, 1.9)
    kv_down = bell_draw(key_of[8], (D_MODEL, KV_RANK), D_MODEL ** -0.5, 0.125)
    kv_gain = jnp.clip(1.0 + 0.18 * jax.random.normal(key_of[9], (KV_RANK,), jnp.float32), 0.1, 1.9)
    rope_down = bell_draw(key_of[10], (D_MODEL, ROPE_DIM), D_MODEL ** -0.5, 0.125)
    query_up = bell_draw(key_of[11], (Q_RANK, HEADS * QK_DIM), Q_RANK ** -0.5, 0.25, ((1, 4),))
    key_up = bell_draw(key_of[12], (KV_RANK, HEADS * NOPE_DIM), KV_RANK ** -0.5, 0.375, ((1, 4),))
    value_up = bell_draw(key_of[13], (KV_RANK, HEADS * VALUE_DIM), KV_RANK ** -0.5, 0.375, ((1, 4),))
    query_norm_gain = draw_query_norm_gain(jax.random.fold_in(key_of[20], 71), part)
    key_norm_gain = draw_key_norm_gain(jax.random.fold_in(key_of[20], 71), part)
    out_weight = bell_draw(key_of[16], (HEADS * VALUE_DIM, D_MODEL), (HEADS * VALUE_DIM) ** -0.5, 0.1875, ((0, 4),))
    context_latent = bell_draw(part_keys[17], (CONTEXT, KV_RANK), 1.0, 6.0, ((0, 4),))
    context_rope = bell_draw(part_keys[18], (CONTEXT, ROPE_DIM), 1.0, 6.0, ((0, 4),))
    context_lift = jnp.clip(2.0 * jax.random.uniform(key_of[19], (HEADS,), jnp.float32) ** block_scale(key_of[19], (HEADS,), ((0, 4),), -0.2, 0.2), 0.0, 2.0)
    return {"latent_tokens": latent_tokens, "condition": condition, "shift_weight": shift_weight, "scale_weight": scale_weight, "gate_weight": gate_weight, "norm_gain": norm_gain, "query_down": query_down, "query_gain": query_gain, "kv_down": kv_down, "kv_gain": kv_gain, "rope_down": rope_down, "query_up": query_up, "key_up": key_up, "value_up": value_up, "query_norm_gain": query_norm_gain, "key_norm_gain": key_norm_gain, "out_weight": out_weight, "context_latent": context_latent, "context_rope": context_rope, "context_lift": context_lift}


EPS = 1e-06
THETA = 10000.0

def rms_scaled(values, gain_vector):
    mean_square = lax.optimization_barrier(jnp.mean(values * values, axis=-1, keepdims=True))
    return values * lax.rsqrt(mean_square + EPS) * gain_vector

def rotate(rope_part, positions):
    row_count = rope_part.shape[0]
    freq_count = ROPE_DIM // 4
    inverse = THETA ** (-4.0 * jnp.arange(freq_count, dtype=jnp.float32) / ROPE_DIM)
    grid_row = (positions // GRID_W).astype(jnp.float32)
    grid_col = (positions % GRID_W).astype(jnp.float32)
    angles = jnp.stack([grid_row[:, None] * inverse, grid_col[:, None] * inverse], axis=1)
    cosine_table = jnp.cos(angles)[:, None]
    sine_table = jnp.sin(angles)[:, None]
    split_rows = rope_part.reshape(row_count, rope_part.shape[1], 2, 2, freq_count)
    first_half = split_rows[:, :, :, 0]
    second_half = split_rows[:, :, :, 1]
    turned = jnp.stack([first_half * cosine_table - second_half * sine_table, second_half * cosine_table + first_half * sine_table], axis=3)
    return turned.reshape(rope_part.shape)

def expand(latent_rows, rope_rows, key_up, value_up, key_norm_gain):
    row_count = latent_rows.shape[0]
    nope_part = jnp.dot(latent_rows, key_up, preferred_element_type=jnp.float32).reshape(row_count, HEADS, NOPE_DIM)
    value_rows = jnp.dot(latent_rows, value_up, preferred_element_type=jnp.float32).astype(jnp.bfloat16)
    shared = jnp.broadcast_to(rope_rows.astype(jnp.float32)[:, None, :], (row_count, HEADS, ROPE_DIM))
    normal_keys = rms_scaled(jnp.concatenate([nope_part, shared], axis=-1), key_norm_gain)
    return (normal_keys, value_rows.reshape(row_count, HEADS, VALUE_DIM))

def reference(latent_tokens, condition, shift_weight, scale_weight, gate_weight, norm_gain, query_down, query_gain, kv_down, kv_gain, rope_down, query_up, key_up, value_up, query_norm_gain, key_norm_gain, out_weight, context_latent, context_rope, context_lift):
    activated = jax.nn.silu(condition.astype(jnp.float32)).astype(jnp.bfloat16)[None]
    mod_shift = jnp.dot(activated, shift_weight, preferred_element_type=jnp.float32)[0]
    mod_scale = jnp.dot(activated, scale_weight, preferred_element_type=jnp.float32)[0]
    mod_gate = jnp.dot(activated, gate_weight, preferred_element_type=jnp.float32)[0]
    token_values = latent_tokens.astype(jnp.float32)
    normed = (rms_scaled(token_values, norm_gain) * (1.0 + mod_scale) + mod_shift).astype(jnp.bfloat16)
    query_latent = rms_scaled(jnp.dot(normed, query_down, preferred_element_type=jnp.float32), query_gain).astype(jnp.bfloat16)
    key_latent = rms_scaled(jnp.dot(normed, kv_down, preferred_element_type=jnp.float32), kv_gain).astype(jnp.bfloat16)
    rope_key = jnp.dot(normed, rope_down, preferred_element_type=jnp.float32).astype(jnp.bfloat16)
    positions = jnp.arange(TOKENS, dtype=jnp.int32)
    query_heads = rms_scaled(jnp.dot(query_latent, query_up, preferred_element_type=jnp.float32).reshape(TOKENS, HEADS, QK_DIM), query_norm_gain)
    queries = jnp.concatenate([query_heads[..., :NOPE_DIM], rotate(query_heads[..., NOPE_DIM:], positions)], axis=-1).astype(jnp.bfloat16)
    latent_normal, latent_values = expand(key_latent, rope_key, key_up, value_up, key_norm_gain)
    latent_keys = jnp.concatenate([latent_normal[..., :NOPE_DIM], rotate(latent_normal[..., NOPE_DIM:], positions)], axis=-1).astype(jnp.bfloat16)
    context_normal, context_values = expand(context_latent, context_rope, key_up, value_up, key_norm_gain)
    context_keys = context_normal.astype(jnp.bfloat16)
    all_keys = jnp.concatenate([latent_keys, context_keys], axis=0)
    all_values = jnp.concatenate([latent_values, context_values], axis=0)
    is_context = jnp.arange(TOKENS + CONTEXT, dtype=jnp.int32) >= TOKENS

    def one_head(inputs):
        query_head, key_head, value_head, lift_head = inputs
        scores = jnp.dot(query_head, key_head.T, preferred_element_type=jnp.float32) * QK_DIM ** (-0.5)
        scores = scores + jnp.where(is_context, lift_head, jnp.zeros((), jnp.float32))[None, :]
        top_score = lax.optimization_barrier(jnp.max(scores, axis=-1, keepdims=True))
        weights = jnp.exp(scores - top_score)
        weight_total = lax.optimization_barrier(jnp.sum(weights, axis=-1, keepdims=True))
        summed = jnp.dot(weights.astype(jnp.bfloat16), value_head, preferred_element_type=jnp.float32)
        return (summed / weight_total).astype(jnp.bfloat16)
    attended = lax.map(one_head, (jnp.transpose(queries, (1, 0, 2)), jnp.transpose(all_keys, (1, 0, 2)), jnp.transpose(all_values, (1, 0, 2)), context_lift))
    attended = jnp.transpose(attended, (1, 0, 2)).reshape(TOKENS, HEADS * VALUE_DIM)
    group_width = HEADS // N_TP * VALUE_DIM
    mixed_sum = jnp.zeros((TOKENS, D_MODEL), jnp.float32)
    for head_group in range(N_TP):
        group_term = jnp.dot(attended[:, head_group * group_width:(head_group + 1) * group_width], out_weight[head_group * group_width:(head_group + 1) * group_width], preferred_element_type=jnp.float32)
        rounded = lax.optimization_barrier(group_term.astype(jnp.bfloat16))
        mixed_sum = mixed_sum + rounded.astype(jnp.float32)
    return (token_values + mod_gate * mixed_sum).astype(jnp.bfloat16)
```

```python
import functools

import jax
import jax.numpy as jnp
import numpy as np
from jax import lax
from jax.experimental import pallas as pl
from jax.experimental.pallas import tpu as pltpu
from jax.sharding import PartitionSpec as P

NOPE_DIM = 64
ROPE_DIM = 32
VALUE_DIM = 64
QK_DIM = 96
GRID_W = 64
LANES = 128

EPS = 1e-06
THETA = 10000.0
LOG2E = 1.4426950408889634
MESH = pl.DeviceIdType.MESH
VMEM_SPEC = pl.BlockSpec(memory_space=pltpu.VMEM)
ANY_SPEC = pl.BlockSpec(memory_space=pl.ANY)
BF16 = jnp.bfloat16
F32 = jnp.float32


def partner_order():
    return np.arange(ROPE_DIM) ^ (ROPE_DIM // 4)


def rope_spread():
    spread = np.zeros((ROPE_DIM, LANES), np.float32)
    order = partner_order()
    for j in range(ROPE_DIM):
        spread[j, NOPE_DIM + j] = 1.0
        spread[order[j], QK_DIM + j] = 1.0
    return spread


def query_spread(heads):
    spread = np.zeros((heads * QK_DIM, heads * LANES), np.float32)
    order = partner_order()
    for h in range(heads):
        for j in range(QK_DIM):
            spread[h * QK_DIM + j, h * LANES + j] = 1.0
        for j in range(ROPE_DIM):
            spread[h * QK_DIM + NOPE_DIM + order[j], h * LANES + QK_DIM + j] = 1.0
    return spread


def head_spread(heads, width):
    spread = np.zeros((heads * width, heads * LANES), np.float32)
    for h in range(heads):
        for j in range(width):
            spread[h * width + j, h * LANES + j] = 1.0
    return spread


def turn_tables(count, axis):
    freq_count = ROPE_DIM // 4
    inverse = np.float32(THETA) ** (-np.float32(4.0) * np.arange(freq_count, dtype=np.float32) / np.float32(ROPE_DIM))
    angles = np.arange(count, dtype=np.float32)[:, None] * inverse.astype(np.float32)
    cosine = np.zeros((count, LANES), np.float32)
    sine = np.zeros((count, LANES), np.float32)
    start = NOPE_DIM + axis * 2 * freq_count
    mid = start + freq_count
    cosine[:, start:mid] = np.cos(angles.astype(np.float64))
    cosine[:, mid : mid + freq_count] = np.cos(angles.astype(np.float64))
    sine[:, start:mid] = -np.sin(angles.astype(np.float64))
    sine[:, mid : mid + freq_count] = np.sin(angles.astype(np.float64))
    if axis == 0:
        cosine[:, :NOPE_DIM] = 1.0
    return cosine, sine


def norm_factor(values):
    return lax.rsqrt(jnp.mean(values * values, axis=-1, keepdims=True) + EPS)


def front_kernel(
    sp, tp,
    cond_ref, shift_w, scale_w, gate_w, tokens_ref, gain_ref, qd_ref, qg_ref, kd_ref, kg_ref, rd_ref,
    cl_ref, cr_ref, spread_ref,
    q_out, kv_out, ctx_out, gate_out,
    mods, q_own, kv_own, ctx_own,
    mod_send, mod_recv, q_send, q_recv, kv_send, kv_recv, c_send, c_recv, local_sem,
):
    s_me = lax.axis_index("sp")
    t_me = lax.axis_index("tp")
    me = s_me * tp + t_me
    half = mods.shape[2]
    rank = cl_ref.shape[1]

    def peer(ds, dt):
        return lax.rem(s_me + ds, sp), lax.rem(t_me + dt, tp)

    others = [(ds, dt) for ds in range(sp) for dt in range(tp) if ds or dt]
    barrier = pltpu.get_barrier_semaphore()
    for ds, dt in others:
        ps, pt = peer(ds, dt)
        pl.semaphore_signal(barrier, inc=1, device_id={"sp": ps, "tp": pt}, device_id_type=MESH)

    c = cond_ref[...].astype(F32)
    act = (c / (1.0 + jnp.exp(-c))).astype(BF16)
    act = jnp.broadcast_to(act, (16, act.shape[1]))
    rows = []
    for w in (shift_w, scale_w, gate_w):
        term = jnp.dot(act, w[...], preferred_element_type=F32)[0:1]
        rows += [term[:, :half], term[:, half:]]
    mods[me] = jnp.concatenate(rows + [rows[0], rows[0]], axis=0)

    spread = spread_ref[...]
    ctx_own[:, :rank] = cl_ref[...]
    ctx_own[:, rank:] = jnp.dot(cr_ref[...], spread, preferred_element_type=F32).astype(BF16)

    pl.semaphore_wait(barrier, len(others))
    copies = []
    mod_copies = []
    for i, (ds, dt) in enumerate(others):
        ps, pt = peer(ds, dt)
        cp = pltpu.make_async_remote_copy(
            src_ref=mods.at[me], dst_ref=mods.at[me], send_sem=mod_send.at[i], recv_sem=mod_recv.at[i],
            device_id={"sp": ps, "tp": pt}, device_id_type=MESH,
        )
        cp.start()
        mod_copies.append(cp)
    for ds in range(1, sp):
        ps, pt = peer(ds, 0)
        cp = pltpu.make_async_remote_copy(
            src_ref=ctx_own, dst_ref=ctx_out.at[s_me], send_sem=c_send.at[ds - 1], recv_sem=c_recv.at[ds - 1],
            device_id={"sp": ps, "tp": pt}, device_id_type=MESH,
        )
        cp.start()
        copies.append(cp)
    own = [pltpu.make_async_copy(ctx_own, ctx_out.at[s_me], local_sem.at[0])]
    own[0].start()

    x = tokens_ref[...].astype(F32)
    xn = x * norm_factor(x) * gain_ref[...]

    for cp in mod_copies:
        cp.wait_recv()
    pieces = [[], [], []]
    for t in range(tp):
        total = mods[t]
        for s in range(1, sp):
            total = total + mods[s * tp + t]
        for k in range(3):
            pieces[k] += [total[2 * k : 2 * k + 1], total[2 * k + 1 : 2 * k + 2]]
    shift, scale, gate = [jnp.concatenate(p, axis=1) for p in pieces]
    gate_out[...] = gate
    normed = (xn * (1.0 + scale) + shift).astype(BF16)

    q = jnp.dot(normed, qd_ref[...], preferred_element_type=F32)
    q_own[...] = (q * norm_factor(q) * qg_ref[...]).astype(BF16)
    kv = jnp.dot(normed, kd_ref[...], preferred_element_type=F32)
    kv_own[:, :rank] = (kv * norm_factor(kv) * kg_ref[...]).astype(BF16)
    rope = jnp.dot(normed, rd_ref[...], preferred_element_type=F32).astype(BF16)
    kv_own[:, rank:] = jnp.dot(rope, spread, preferred_element_type=F32).astype(BF16)

    for dt in range(1, tp):
        ps, pt = peer(0, dt)
        cp = pltpu.make_async_remote_copy(
            src_ref=q_own, dst_ref=q_out.at[t_me], send_sem=q_send.at[dt - 1], recv_sem=q_recv.at[dt - 1],
            device_id={"sp": ps, "tp": pt}, device_id_type=MESH,
        )
        cp.start()
        copies.append(cp)
    for i, (ds, dt) in enumerate(others):
        ps, pt = peer(ds, dt)
        cp = pltpu.make_async_remote_copy(
            src_ref=kv_own, dst_ref=kv_out.at[me], send_sem=kv_send.at[i], recv_sem=kv_recv.at[i],
            device_id={"sp": ps, "tp": pt}, device_id_type=MESH,
        )
        cp.start()
        copies.append(cp)
    own.append(pltpu.make_async_copy(q_own, q_out.at[t_me], local_sem.at[1]))
    own.append(pltpu.make_async_copy(kv_own, kv_out.at[me], local_sem.at[2]))
    own[1].start()
    own[2].start()
    for cp in mod_copies:
        cp.wait_send()
    for cp in copies:
        cp.wait()
    for cp in own:
        cp.wait()


def attend_kernel(
    heads, s_ref, q_ref, kv_ref, ctx_ref, qu_ref, ku_ref, vu_ref, qe_ref, ke_ref, ve_ref,
    qgain_ref, kgain_ref, lift_ref, row_a, row_b, col_a, col_b, out_ref,
    k_lat, v_lat, k_ctx, v_ctx, q_all,
):
    rank = ku_ref.shape[0]
    tokens = kv_ref.shape[0]
    group = q_ref.shape[0]
    context = ctx_ref.shape[0]
    lane = lax.broadcasted_iota(jnp.int32, (1, LANES), 1)
    live = lane < QK_DIM
    ones_lane = jnp.where(lane == VALUE_DIM, 1.0, 0.0).astype(F32)
    qu = jnp.dot(qu_ref[...], qe_ref[...], preferred_element_type=F32).astype(BF16)
    ku = jnp.dot(ku_ref[...], ke_ref[...], preferred_element_type=F32).astype(BF16)
    vu = jnp.dot(vu_ref[...], ve_ref[...], preferred_element_type=F32).astype(BF16)

    def tables(first_row, row_count, gain):
        gain_partner = pltpu.roll(gain, QK_DIM, 1)
        a = [(row_a[pl.ds(first_row + r, 1), :] + col_a[...]) * gain[0:1] for r in range(row_count)]
        b = [(row_b[pl.ds(first_row + r, 1), :] + col_b[...]) * gain_partner[0:1] for r in range(row_count)]
        return jnp.concatenate(a, axis=0), jnp.concatenate(b, axis=0)

    def finish(v, a, b):
        square = jnp.where(live, v * v, 0.0)
        factor = lax.rsqrt(jnp.sum(square, axis=-1, keepdims=True) * (1.0 / QK_DIM) + EPS)
        if b is None:
            return (v * a * factor).astype(BF16)
        return ((v * a + pltpu.roll(v, QK_DIM, 1) * b) * factor).astype(BF16)

    block = min(256, group)
    grid_rows = block // GRID_W
    qgain = qgain_ref[...]
    kgain = kgain_ref[...]

    def query_block(i, carry):
        start = pl.multiple_of(i * block, block)
        q = jnp.dot(q_ref[pl.ds(start, block), :], qu, preferred_element_type=F32)
        a, b = tables(s_ref[0] * (group // GRID_W) + i * grid_rows, grid_rows, qgain)
        for h in range(heads):
            q_all[h, pl.ds(start, block), :] = finish(q[:, h * LANES : (h + 1) * LANES], a, b)
        return carry

    lax.fori_loop(0, group // block, query_block, 0)

    def key_block(i, carry):
        start = pl.multiple_of(i * block, block)
        lat = kv_ref[pl.ds(start, block), :rank]
        rope = kv_ref[pl.ds(start, block), rank:].astype(F32)
        k = jnp.dot(lat, ku, preferred_element_type=F32)
        v = jnp.dot(lat, vu, preferred_element_type=F32)
        a, b = tables(i * grid_rows, grid_rows, kgain)
        for h in range(heads):
            k_lat[h, pl.ds(start, block), :] = finish(k[:, h * LANES : (h + 1) * LANES] + rope, a, b)
            v_lat[h, pl.ds(start, block), :] = (v[:, h * LANES : (h + 1) * LANES] + ones_lane).astype(BF16)
        return carry

    lax.fori_loop(0, tokens // block, key_block, 0)
    plain = jnp.where(live, kgain[0:1], 0.0)

    def context_block(i, carry):
        start = pl.multiple_of(i * block, block)
        lat = ctx_ref[pl.ds(start, block), :rank]
        rope = ctx_ref[pl.ds(start, block), rank:].astype(F32)
        k = jnp.dot(lat, ku, preferred_element_type=F32)
        v = jnp.dot(lat, vu, preferred_element_type=F32)
        for h in range(heads):
            k_ctx[h, pl.ds(start, block), :] = finish(k[:, h * LANES : (h + 1) * LANES] + rope, plain, None)
            v_ctx[h, pl.ds(start, block), :] = (v[:, h * LANES : (h + 1) * LANES] + ones_lane).astype(BF16)
        return carry

    lax.fori_loop(0, context // block, context_block, 0)

    factor = LOG2E * QK_DIM ** (-0.5)
    contract = (((1,), (1,)), ((), ()))
    q_rows = min(256, group)

    def attend(i, carry):
        start = pl.multiple_of(i * q_rows, q_rows)
        outs = []
        for h in range(heads):
            q = q_all[h, pl.ds(start, q_rows), :]
            s_lat = lax.dot_general(q, k_lat[h], contract, preferred_element_type=F32)
            s_ctx = lax.dot_general(q, k_ctx[h], contract, preferred_element_type=F32)
            lift = lift_ref[h] * LOG2E
            top = jnp.maximum(
                jnp.max(s_lat, axis=-1, keepdims=True) * factor,
                jnp.max(s_ctx, axis=-1, keepdims=True) * factor + lift,
            )
            p_lat = jnp.exp2(s_lat * factor - top).astype(BF16)
            p_ctx = jnp.exp2(s_ctx * factor - (top - lift)).astype(BF16)
            acc = jnp.dot(p_lat, v_lat[h], preferred_element_type=F32) + jnp.dot(
                p_ctx, v_ctx[h], preferred_element_type=F32
            )
            outs.append((acc[:, :VALUE_DIM] / acc[:, VALUE_DIM : VALUE_DIM + 1]).astype(BF16))
        out_ref[pl.ds(start, q_rows), :] = jnp.concatenate(outs, axis=1)
        return carry

    lax.fori_loop(0, group // q_rows, attend, 0)


def tail_kernel(tp, att_ref, tokens_ref, gate_ref, *rest):
    weights = rest[:tp]
    out_ref, held, send_sem, recv_sem = rest[tp:]
    t_me = lax.axis_index("tp")
    rows = tokens_ref.shape[0]
    barrier = pltpu.get_barrier_semaphore()
    for dt in range(1, tp):
        pl.semaphore_signal(barrier, inc=1, device_id={"tp": lax.rem(t_me + dt, tp)}, device_id_type=MESH)
    pl.semaphore_wait(barrier, tp - 1)
    copies = []
    for dt in range(1, tp):
        dest = lax.rem(t_me + dt, tp)
        cp = pltpu.make_async_remote_copy(
            src_ref=att_ref.at[dest], dst_ref=held.at[dt - 1],
            send_sem=send_sem.at[dt - 1], recv_sem=recv_sem.at[dt - 1],
            device_id={"tp": dest}, device_id_type=MESH,
        )
        cp.start()
        copies.append(cp)
    chunk = 512
    width = out_ref.shape[1]
    gate = gate_ref[...]
    for dt in range(1, tp):
        copies[dt - 1].wait()
    for n in range(width // chunk):
        cols = slice(n * chunk, (n + 1) * chunk)
        mixed = jnp.dot(att_ref[t_me], weights[0][:, cols], preferred_element_type=F32).astype(BF16).astype(F32)
        for dt in range(1, tp):
            mixed = mixed + jnp.dot(
                held[dt - 1], weights[dt][:, cols], preferred_element_type=F32
            ).astype(BF16).astype(F32)
        out_ref[:, cols] = (tokens_ref[:, cols].astype(F32) + gate[:, cols] * mixed).astype(BF16)


def local(
    sp, tp, dp,
    latent_tokens, condition, shift_weight, scale_weight, gate_weight, norm_gain,
    query_down, query_gain, kv_down, kv_gain, rope_down, query_up, key_up, value_up,
    query_norm_gain, key_norm_gain, out_weight, context_latent, context_rope, context_lift,
):
    rows, width = latent_tokens.shape
    q_rank = query_down.shape[1]
    rank = kv_down.shape[1]
    heads = query_up.shape[1] // QK_DIM
    ctx_rows = context_latent.shape[0]
    group = rows * tp
    tokens = group * sp
    n_dev = sp * tp

    k_rows = out_weight.shape[0]
    half = k_rows // dp
    d_me = lax.axis_index("dp")
    mine = lax.dynamic_slice_in_dim(out_weight, d_me * half, half, axis=0)
    weights = [out_weight]
    for dt in range(1, tp):
        got = lax.ppermute(mine, "tp", [(i, (i + dt) % tp) for i in range(tp)])
        other = lax.ppermute(got, "dp", [(i, (i + 1) % dp) for i in range(dp)])
        weights.append((got, other))

    front = pl.pallas_call(
        functools.partial(front_kernel, sp, tp),
        out_shape=(
            jax.ShapeDtypeStruct((tp, rows, q_rank), BF16),
            jax.ShapeDtypeStruct((n_dev, rows, rank + LANES), BF16),
            jax.ShapeDtypeStruct((sp, ctx_rows, rank + LANES), BF16),
            jax.ShapeDtypeStruct((1, width), F32),
        ),
        in_specs=[VMEM_SPEC] * 14,
        out_specs=(ANY_SPEC, ANY_SPEC, ANY_SPEC, VMEM_SPEC),
        scratch_shapes=[
            pltpu.VMEM((n_dev, 8, width // tp // 2), F32),
            pltpu.VMEM((rows, q_rank), BF16),
            pltpu.VMEM((rows, rank + LANES), BF16),
            pltpu.VMEM((ctx_rows, rank + LANES), BF16),
            pltpu.SemaphoreType.DMA((n_dev - 1,)),
            pltpu.SemaphoreType.DMA((n_dev - 1,)),
            pltpu.SemaphoreType.DMA((tp - 1,)),
            pltpu.SemaphoreType.DMA((tp - 1,)),
            pltpu.SemaphoreType.DMA((n_dev - 1,)),
            pltpu.SemaphoreType.DMA((n_dev - 1,)),
            pltpu.SemaphoreType.DMA((sp - 1,)),
            pltpu.SemaphoreType.DMA((sp - 1,)),
            pltpu.SemaphoreType.DMA((3,)),
        ],
        compiler_params=pltpu.CompilerParams(
            collective_id=0, has_side_effects=True, vmem_limit_bytes=32 * 1024 * 1024
        ),
        cost_estimate=pl.CostEstimate(flops=20_000_000_000, bytes_accessed=8_000_000, transcendentals=0),
        name="front",
    )
    q_group, kv_all, ctx_all, mod_gate = front(
        condition[None], shift_weight, scale_weight, gate_weight, latent_tokens, norm_gain[None],
        query_down, query_gain[None], kv_down, kv_gain[None], rope_down,
        context_latent, context_rope, jnp.asarray(rope_spread(), BF16),
    )

    def extended(gain):
        freq = ROPE_DIM // 4
        parts = [gain]
        for axis in range(2):
            start = NOPE_DIM + axis * 2 * freq
            parts += [gain[start + freq : start + 2 * freq], gain[start : start + freq]]
        return jnp.broadcast_to(jnp.concatenate(parts)[None], (8, LANES))

    row_a, row_b = turn_tables(tokens // GRID_W, 0)
    col_a, col_b = turn_tables(GRID_W, 1)
    context = sp * ctx_rows
    smem = pl.BlockSpec(memory_space=pltpu.SMEM)
    attended = pl.pallas_call(
        functools.partial(attend_kernel, heads),
        out_shape=jax.ShapeDtypeStruct((group, heads * VALUE_DIM), BF16),
        in_specs=[smem] + [VMEM_SPEC] * 11 + [smem] + [VMEM_SPEC] * 4,
        out_specs=VMEM_SPEC,
        scratch_shapes=[
            pltpu.VMEM((heads, tokens, LANES), BF16),
            pltpu.VMEM((heads, tokens, LANES), BF16),
            pltpu.VMEM((heads, context, LANES), BF16),
            pltpu.VMEM((heads, context, LANES), BF16),
            pltpu.VMEM((heads, group, LANES), BF16),
        ],
        compiler_params=pltpu.CompilerParams(vmem_limit_bytes=60 * 1024 * 1024),
        cost_estimate=pl.CostEstimate(flops=20_000_000_000, bytes_accessed=8_000_000, transcendentals=0),
        name="attend",
    )(
        lax.axis_index("sp").astype(jnp.int32)[None],
        q_group.reshape(group, q_rank), kv_all.reshape(tokens, rank + LANES),
        ctx_all.reshape(context, rank + LANES), query_up, key_up, value_up,
        jnp.asarray(query_spread(heads), BF16), jnp.asarray(head_spread(heads, NOPE_DIM), BF16),
        jnp.asarray(head_spread(heads, VALUE_DIM), BF16),
        extended(query_norm_gain), extended(key_norm_gain), context_lift,
        jnp.asarray(row_a), jnp.asarray(row_b), jnp.asarray(col_a), jnp.asarray(col_b),
    )

    full = [out_weight]
    for got, other in weights[1:]:
        low = jnp.where(d_me == 0, got, other)
        high = jnp.where(d_me == 0, other, got)
        full.append(jnp.concatenate([low, high], axis=0))
    return pl.pallas_call(
        functools.partial(tail_kernel, tp),
        out_shape=jax.ShapeDtypeStruct((rows, width), BF16),
        in_specs=[VMEM_SPEC] * (3 + tp),
        out_specs=VMEM_SPEC,
        scratch_shapes=[
            pltpu.VMEM((tp - 1, rows, heads * VALUE_DIM), BF16),
            pltpu.SemaphoreType.DMA((tp - 1,)),
            pltpu.SemaphoreType.DMA((tp - 1,)),
        ],
        compiler_params=pltpu.CompilerParams(
            collective_id=1, has_side_effects=True, vmem_limit_bytes=32 * 1024 * 1024
        ),
        name="tail",
    )(attended.reshape(tp, rows, heads * VALUE_DIM), latent_tokens, mod_gate, *full)


def solution(mesh):
    in_specs = (
        P(("dp", "sp", "tp"), None), P(("dp", "sp")), P("sp", "tp"), P("sp", "tp"), P("sp", "tp"),
        P(), P(), P(), P(), P(), P(), P(None, "tp"), P(None, "tp"), P(None, "tp"), P(), P(),
        P("tp", None), P(("dp", "sp"), None), P(("dp", "sp"), None), P("tp"),
    )
    out_specs = P(("dp", "sp", "tp"), None)
    body = functools.partial(local, mesh.shape["sp"], mesh.shape["tp"], mesh.shape["dp"])
    return jax.shard_map(body, mesh=mesh, in_specs=in_specs, out_specs=out_specs, check_vma=False)
```
